32 devices in a mesh: sp: 8 (over z, y), tp: 4 (over x, core).
Axes of the slice: x: 2, y: 2, z: 4, core: 2. Of those that a mesh axis runs over, the one named last changes fastest.
Arguments:
- tokens: bfloat16 [1024, 2048], P(('sp', 'tp')), may hold values from -6 to 6
- norm_gain: float32 [2048], replicated, may hold values from 0.1 to 1.9
- w_filter_b: bfloat16 [2048, 1024], P('sp', 'tp'), may hold values from -0.125 to 0.125
- w_filter_c: bfloat16 [2048, 1024], P('sp', 'tp'), may hold values from -0.125 to 0.125
- w_filter_v: bfloat16 [2048, 1024], P('sp', 'tp'), may hold values from -0.125 to 0.125
- filter_taps: float32 [3, 1024], P(None, 'tp'), may hold values from -3.5 to 3.5
- w_query: bfloat16 [2048, 1024], P('sp', 'tp'), may hold values from -0.125 to 0.125
- retention_gate_matrix: bfloat16 [2048, 1024], P('sp', 'tp'), may hold values from -0.125 to 0.125
- w_input: bfloat16 [2048, 1024], P('sp', 'tp'), may hold values from -0.125 to 0.125
- forget_gap: float32 [1024], P('tp'), may hold values from 0 to 0.12
- additive_fade_log: float32 [1024, 1024], P('sp', 'tp'), may hold values from -1.1 to 0
- head_gain: float32 [128], replicated, may hold values from 0.1 to 1.9
- initial_state: float32 [8, 128, 128], P('tp'), may hold values from -0.0546875 to 0.0546875
- w_out_filter: bfloat16 [1024, 2048], P('tp'), may hold values from -0.125 to 0.125
- w_out_rec: bfloat16 [1024, 2048], P('tp'), may hold values from -0.125 to 0.125
Outputs:
- mixed: bfloat16 [1024, 2048], P(('sp', 'tp'))
The draws below stay inside these ranges and needn't reach their ends.
All inputs are finite; a program needn't handle non-finite values.
Results may differ from the reference program's by a relative error of at most 0.03.
Values may be sent and summed in bfloat16 or wider, within the bound.
A program may use at most 64 MiB of HBM per device.

```python
import math
import jax
import jax.numpy as jnp
from jax import lax

D = 2048
CONV = 1024
HEADS = 8
HEAD_DIM = 128
SPAN = 64
TAPS = 3
TOK_DEV = 128
FEATURE_SPAN = 1024
SEQUENCE_SIZE = 1024
N_TP = 4


def draw_forget_gap(key, part):
    order_key, fast_key, slow_key = jax.random.split(jax.random.fold_in(key, 11), 3)
    slow_count = HEADS // 2
    ranking = jax.random.permutation(order_key, HEADS)
    slow_head = ranking < slow_count
    fast_gap = jnp.exp(jax.random.uniform(fast_key, (HEADS, HEAD_DIM), jnp.float32, math.log(0.04), math.log(0.12)))
    slow_gap = jnp.exp(jax.random.uniform(slow_key, (HEADS, HEAD_DIM), jnp.float32, math.log(0.2), math.log(0.6))) / SEQUENCE_SIZE
    return jnp.where(slow_head[:, None], slow_gap, fast_gap).reshape(HEADS * HEAD_DIM)


def draw_additive_fade_log(key, part):
    rate_key, factor_key, spot_key, loss_key = jax.random.split(jax.random.fold_in(key, 23), 4)
    low_factor, high_factor = (0.5, 2.0)
    base_rate = jnp.exp(jax.random.uniform(rate_key, (FEATURE_SPAN,), jnp.float32, math.log(0.1), math.log(0.4))) / SEQUENCE_SIZE
    segments = SEQUENCE_SIZE // TOK_DEV
    factor = jnp.exp(jax.random.uniform(factor_key, (segments, 1, FEATURE_SPAN), jnp.float32, math.log(low_factor), math.log(high_factor)))
    settled_memory = -(base_rate[None, None, :] * factor) * jnp.ones((1, TOK_DEV, 1), jnp.float32)
    spot_rows = jax.random.randint(spot_key, (3,), 0, SEQUENCE_SIZE)
    objective_entries = jax.random.uniform(loss_key, (3,), jnp.float32, 0.2, 0.4)
    indexed_catalog = (jnp.arange(SEQUENCE_SIZE)[:, None] == spot_rows[None, :]).astype(jnp.float32)
    packet_bundles = jnp.sum(indexed_catalog * jnp.log1p(-objective_entries)[None, :], axis=1)
    return settled_memory.reshape(SEQUENCE_SIZE, FEATURE_SPAN) + packet_bundles[:, None]


def shard_levels(stream_key, shape, shards, least, top_value):
    gain = 1.0
    for position, blocks in shards:
        heights = jax.random.uniform(jax.random.fold_in(jax.random.fold_in(stream_key, 6), position), (blocks,), jnp.float32, least / len(shards), top_value / len(shards))
        gain = gain * jnp.repeat(jnp.exp(heights), shape[position] // blocks).reshape((-1,) + (1,) * (len(shape) - 1 - position))
    return gain


def bell_draw(rng, shape, scale, most, cuts=(), held_as=jnp.bfloat16):
    gain = shard_levels(rng, shape, cuts, -0.22, 0.18) if cuts else 1.0
    array = jax.random.normal(rng, shape, jnp.float32) * scale * gain
    return jnp.minimum(jnp.maximum(array, -most), most).astype(held_as)


def setup_inputs(seed: int = 0) -> dict:
    arg_keys = jax.random.split(jax.random.key(seed), 16)
    return {
        "tokens": bell_draw(arg_keys[0], (SEQUENCE_SIZE, D), 1.0, 6.0, ((0, 32),)),
        "norm_gain": jnp.clip(1.0 + 0.18 * jax.random.normal(arg_keys[1], (D,), jnp.float32), 0.1, 1.9),
        "w_filter_b": bell_draw(arg_keys[2], (D, CONV), D ** -0.5, 0.125, ((0, 8), (1, 4))),
        "w_filter_c": bell_draw(arg_keys[3], (D, CONV), D ** -0.5, 0.125, ((0, 8), (1, 4))),
        "w_filter_v": bell_draw(arg_keys[4], (D, CONV), D ** -0.5, 0.125, ((0, 8), (1, 4))),
        "filter_taps": bell_draw(arg_keys[5], (TAPS, CONV), TAPS ** -0.5, 3.5, ((1, 4),), jnp.float32),
        "w_query": bell_draw(arg_keys[6], (D, FEATURE_SPAN), D ** -0.5, 0.125, ((0, 8), (1, 4))),
        "retention_gate_matrix": bell_draw(arg_keys[7], (D, FEATURE_SPAN), D ** -0.5, 0.125, ((0, 8), (1, 4))),
        "w_input": bell_draw(arg_keys[8], (D, FEATURE_SPAN), D ** -0.5, 0.125, ((0, 8), (1, 4))),
        "forget_gap": draw_forget_gap(jax.random.fold_in(arg_keys[15], 71), 0),
        "additive_fade_log": draw_additive_fade_log(jax.random.fold_in(arg_keys[15], 71), 0),
        "head_gain": jnp.clip(1.0 + 0.18 * jax.random.normal(arg_keys[11], (HEAD_DIM,), jnp.float32), 0.1, 1.9),
        "initial_state": bell_draw(arg_keys[12], (HEADS, HEAD_DIM, HEAD_DIM), (0.3 * SEQUENCE_SIZE ** -0.5), 0.0546875, ((0, 4),), jnp.float32),
        "w_out_filter": bell_draw(arg_keys[13], (CONV, D), (CONV + FEATURE_SPAN) ** -0.5, 0.125, ((0, 4),)),
        "w_out_rec": bell_draw(arg_keys[14], (FEATURE_SPAN, D), (CONV + FEATURE_SPAN) ** -0.5, 0.125, ((0, 4),)),
    }


epsilon = 1e-06
highest_precision = lax.Precision.HIGHEST

def block_step(carried_state, inputs):
    block_query, block_key, block_value_rows, block_decay = inputs
    causal = jnp.tril(jnp.ones((SPAN, SPAN), dtype=bool))
    running = jnp.cumsum(block_decay, axis=0)
    scaled_query = block_query * jnp.exp(running)
    key_scaled = block_key * jnp.exp(-running)
    scores = jnp.einsum('thk,shk->hts', scaled_query, key_scaled, precision=highest_precision)
    scores = jnp.where(causal[None], scores, 0.0)
    final_result = jnp.einsum('hts,shv->thv', scores, block_value_rows, precision=highest_precision)
    final_result = final_result + jnp.einsum('oql,qlz->oqz', scaled_query, carried_state, precision=highest_precision)
    final_state = running[-1]
    key_remainder = block_key * jnp.exp(final_state[None] - running)
    updated_state = jnp.exp(final_state)[:, :, None] * carried_state + jnp.einsum('dri,drz->riz', key_remainder, block_value_rows, precision=highest_precision)
    return (updated_state, final_result)

def reference(tokens, norm_gain, w_filter_b, w_filter_c, w_filter_v, filter_taps, w_query, retention_gate_matrix, w_input, forget_gap, additive_fade_log, head_gain, initial_state, w_out_filter, w_out_rec):
    widened = tokens.astype(jnp.float32)
    normed = (widened * lax.rsqrt(lax.optimization_barrier(jnp.mean(widened * widened, axis=-1, keepdims=True)) + epsilon) * norm_gain).astype(jnp.bfloat16)

    def project(weight):
        return jnp.dot(normed, weight, preferred_element_type=jnp.float32).astype(jnp.bfloat16)
    gate_out = project(w_filter_b)
    product = project(w_filter_c).astype(jnp.float32) * project(w_filter_v).astype(jnp.float32)
    padded = jnp.concatenate([jnp.zeros((TAPS - 1, CONV), jnp.float32), product], axis=0)
    filtered = jnp.zeros_like(product)
    for offset in range(TAPS):
        filtered = filtered + filter_taps[offset] * padded[offset:offset + SEQUENCE_SIZE]
    filter_out = (gate_out.astype(jnp.float32) * filtered).astype(jnp.bfloat16)
    queries = project(w_query).astype(jnp.float32)
    forget_logit = project(retention_gate_matrix).astype(jnp.float32)
    input_value = project(w_input).astype(jnp.float32)
    key_rate = forget_gap * jax.nn.sigmoid(-forget_logit)
    log_decay = jnp.log1p(-key_rate) + additive_fade_log
    value_in = jax.nn.silu(input_value)

    def heads_blocks(flat_rows):
        return flat_rows.reshape(SEQUENCE_SIZE // SPAN, SPAN, HEADS, HEAD_DIM)
    ignored_state, unmixed_output = lax.scan(block_step, initial_state, (heads_blocks(queries), heads_blocks(key_rate), heads_blocks(value_in), heads_blocks(log_decay)))
    unmixed_output = unmixed_output.reshape(SEQUENCE_SIZE, HEADS, HEAD_DIM)
    rec_out = (unmixed_output * lax.rsqrt(lax.optimization_barrier(jnp.mean(unmixed_output * unmixed_output, axis=-1, keepdims=True)) + epsilon) * head_gain).astype(jnp.bfloat16).reshape(SEQUENCE_SIZE, FEATURE_SPAN)
    filter_group = CONV // N_TP
    recur_group = FEATURE_SPAN // N_TP
    summed = jnp.zeros((SEQUENCE_SIZE, D), jnp.float32)
    for member in range(N_TP):
        filter_part = filter_out[:, member * filter_group:(member + 1) * filter_group]
        recur_part = rec_out[:, member * recur_group:(member + 1) * recur_group]
        partial_value = jnp.dot(filter_part, w_out_filter[member * filter_group:(member + 1) * filter_group], preferred_element_type=jnp.float32)
        partial_value = partial_value + jnp.dot(recur_part, w_out_rec[member * recur_group:(member + 1) * recur_group], preferred_element_type=jnp.float32)
        rounded = lax.optimization_barrier(partial_value.astype(jnp.bfloat16))
        summed = summed + rounded.astype(jnp.float32)
    return summed.astype(jnp.bfloat16)
```

```python
import functools

import jax
import jax.numpy as jnp
from jax import lax
from jax.experimental import pallas as pl
from jax.experimental.pallas import tpu as pltpu
from jax.sharding import PartitionSpec as P

HEAD_DIM = 128
TAPS = 3
SHARES = 4
CHUNKS = 4
PROJ = 6
EPS = 1e-06
MESH = pl.DeviceIdType.MESH
F32 = jnp.float32
BF16 = jnp.bfloat16


def repeat(count, step):
    if count <= 4:
        for i in range(count):
            step(i)
    else:
        lax.fori_loop(0, count, lambda i, c: (step(i), c)[1], 0)


def dot(a, b):
    return jnp.dot(a, b, preferred_element_type=F32)


def dot_on(a, b, da, db):
    return lax.dot_general(a, b, (((da,), (db,)), ((), ())), preferred_element_type=F32)


def mix_kernel(
    n_sp,
    n_tp,
    tok,
    gain,
    taps,
    gap,
    fade,
    hgain,
    init,
    wq,
    wf,
    wi,
    wc,
    wv,
    wb,
    wof,
    wor,
    out,
    xs,
    xbuf,
    wbuf,
    own,
    psend,
    pland,
    sland,
    gland,
    sin,
    pad,
    obuf,
    oland,
    vof,
    vor,
    tok_s,
    tok_r,
    w_l,
    w_s,
    w_r,
    p_s,
    p_r,
    s_s,
    s_r,
    g_s,
    g_r,
    h_s,
    h_r,
    o_s,
    o_r,
    v_l,
):
    sp, tp = lax.axis_index("sp"), lax.axis_index("tp")
    group = n_sp // SHARES
    z, r = lax.div(sp, group), lax.rem(sp, group)
    t_loc = tok.shape[0]
    length = t_loc * n_tp
    rows, width = wq.shape
    depth = rows * group
    heads = width // HEAD_DIM
    weights = (wq, wf, wi, wc, wv, wb)

    def shift_z(by):
        return lax.rem(z + by + SHARES, SHARES)

    def shift_t(by):
        return lax.rem(tp + by + n_tp, n_tp)

    def shift_r(by):
        return lax.rem(r + by + group, group)

    def send(src, dst, ss, rs, to):
        return pltpu.make_async_remote_copy(
            src_ref=src, dst_ref=dst, send_sem=ss, recv_sem=rs, device_id=to, device_id_type=MESH
        )

    barrier = pltpu.get_barrier_semaphore()

    def hail(a, b):
        pl.semaphore_signal(barrier, inc=1, device_id=(a, b), device_id_type=MESH)

    repeat(group - 1, lambda i: hail(z * group + shift_r(i + 1), tp))
    spread = [(a, b) for a in range(SHARES) for b in range(n_tp) if (a, b) != (0, 0)]
    for a, b in spread:
        hail(shift_z(a) * group + r, shift_t(b))
    after, before = lax.rem(sp + 1, n_sp), lax.rem(sp + n_sp - 1, n_sp)
    hail(after, tp)
    hail(before, tp)

    mine = pl.ds(pl.multiple_of(r * rows, rows), rows)
    for p in range(PROJ):
        pltpu.make_async_copy(weights[p], wbuf.at[p, mine], w_l.at[p]).start()
    pltpu.make_async_copy(wof, vof, v_l.at[0]).start()
    pltpu.make_async_copy(wor, vor, v_l.at[1]).start()

    x = tok[...].astype(F32)
    normed = x * lax.rsqrt(jnp.mean(x * x, axis=-1, keepdims=True) + EPS) * gain[...]
    normed = normed.astype(BF16)
    for a in range(SHARES):
        xs[a] = normed[:, a * depth : (a + 1) * depth]
    xbuf[z, tp] = xs[z]

    pl.semaphore_wait(barrier, group - 1 + len(spread) + 2)

    def token_copy(a, b):
        to = (shift_z(a) * group + r, shift_t(b))
        return send(xs.at[shift_z(a)], xbuf.at[z, tp], tok_s.at[a, b], tok_r.at[a, b], to)

    def token_landing(a, b):
        to = (shift_z(-a) * group + r, shift_t(-b))
        return send(
            xs.at[0], xbuf.at[shift_z(-a), shift_t(-b)], tok_s.at[a, b], tok_r.at[a, b], to
        )

    def weight_copy(p, i):
        to = (z * group + shift_r(i + 1), tp)
        return send(weights[p], wbuf.at[p, mine], w_s.at[p, i], w_r.at[p, i], to)

    def weight_landing(p, i):
        src = shift_r(-i - 1)
        theirs = pl.ds(pl.multiple_of(src * rows, rows), rows)
        return send(
            weights[p], wbuf.at[p, theirs], w_s.at[p, i], w_r.at[p, i], (z * group + src, tp)
        )

    repeat(group - 1, lambda i: weight_copy(0, i).start())
    for a, b in spread:
        token_copy(a, b).start()
    for p in range(1, PROJ):
        repeat(group - 1, lambda i: weight_copy(p, i).start())

    for a, b in spread:
        token_landing(a, b).wait_recv()

    def part_copy(p, a):
        to = (shift_z(a) * group + r, tp)
        return send(psend.at[p, shift_z(a)], pland.at[p, a], p_s.at[p, a], p_r.at[p, a], to)

    def project(p):
        pltpu.make_async_copy(weights[p], wbuf.at[p, mine], w_l.at[p]).wait()
        repeat(group - 1, lambda i: weight_landing(p, i).wait_recv())
        full = xbuf[...].reshape(SHARES * length, depth)
        part = dot(full, wbuf[p]).reshape(SHARES, length, width)
        own[p] = part
        psend[p] = part.astype(BF16)
        for a in (2, 1, 3):
            part_copy(p, a).start()

    def total(p):
        for a in range(1, SHARES):
            part_copy(p, a).wait_recv()
        s = own[p, z]
        for a in range(1, SHARES):
            s = s + pland[p, a].astype(F32)
        return s.astype(BF16).astype(F32)

    for p in range(4):
        project(p)

    query, logit, value = total(0), total(1), total(2)
    rate = gap[...] / (1.0 + jnp.exp(logit))
    decay = jnp.log1p(-rate) + fade[...]
    value = (value / (1.0 + jnp.exp(-value))).astype(BF16)
    below = lax.broadcasted_iota(jnp.int32, (length, length), 0) >= lax.broadcasted_iota(
        jnp.int32, (length, length), 1
    )
    running = jnp.dot(
        below.astype(F32), decay, preferred_element_type=F32, precision=lax.Precision.HIGHEST
    )
    middle = running[length // 2 - 1 : length // 2]
    last = running[length - 1 : length]
    query_mid = (query * jnp.exp(running - middle)).astype(BF16)
    key_mid = (rate * jnp.exp(middle - running)).astype(BF16)
    key_end = (rate * jnp.exp(last - running)).astype(BF16)
    query_in = (query * jnp.exp(running)).astype(BF16)
    within = []
    cuts = [slice(h * HEAD_DIM, (h + 1) * HEAD_DIM) for h in range(heads)]
    for cut in cuts:
        sland[r, 0:HEAD_DIM, cut] = dot_on(value[:, cut], key_end[:, cut], 0, 0).astype(BF16)
    coarse = last.astype(BF16).astype(F32)
    upper = lax.broadcasted_iota(jnp.int32, (16, width), 0) < 8
    sland[r, HEAD_DIM : HEAD_DIM + 16, :] = jnp.where(upper, coarse, last - coarse).astype(BF16)

    def state_copy(i):
        to = (z * group + shift_r(i + 1), tp)
        return send(sland.at[r], sland.at[r], s_s.at[i], s_r.at[i], to)

    def state_landing(i):
        src = shift_r(-i - 1)
        return send(sland.at[src], sland.at[src], s_s.at[i], s_r.at[i], (z * group + src, tp))

    repeat(group - 1, lambda i: state_copy(i).start())
    for cut in cuts:
        scores = dot_on(query_mid[:, cut], key_mid[:, cut], 1, 1)
        scores = jnp.where(below, scores, 0.0).astype(BF16)
        within.append(dot(scores, value[:, cut]))

    for p in range(4, PROJ):
        project(p)

    repeat(group - 1, lambda i: state_landing(i).wait_recv())

    def parts_of(ref, i):
        tail = ref[i, HEAD_DIM : HEAD_DIM + 16, :].astype(F32)
        return ref[i, 0:HEAD_DIM, :].astype(F32), tail[0:1] + tail[8:9]

    def join(i, carry):
        whole, whole_decay, near, near_decay = carry
        state, fall = parts_of(sland, i)
        factor = jnp.exp(fall)
        whole, whole_decay = factor * whole + state, whole_decay + fall
        earlier = i < r
        near = jnp.where(earlier, factor * near + state, near)
        near_decay = jnp.where(earlier, near_decay + fall, near_decay)
        return whole, whole_decay, near, near_decay

    blank = jnp.zeros((HEAD_DIM, width), F32)
    line = jnp.zeros((1, width), F32)
    carry = (blank, line, blank, line)
    if group <= 4:
        for i in range(group):
            carry = join(i, carry)
    else:
        carry = lax.fori_loop(0, group, join, carry)
    whole, whole_decay, near, near_decay = carry
    gland[z, 0:HEAD_DIM, :] = whole.astype(BF16)
    coarse = whole_decay.astype(BF16).astype(F32)
    gland[z, HEAD_DIM : HEAD_DIM + 16, :] = jnp.where(upper, coarse, whole_decay - coarse).astype(
        BF16
    )

    def group_copy(a):
        return send(
            gland.at[z], gland.at[z], g_s.at[a], g_r.at[a], (shift_z(a) * group + r, tp)
        )

    def group_landing(a):
        src = shift_z(-a)
        return send(gland.at[src], gland.at[src], g_s.at[a], g_r.at[a], (src * group + r, tp))

    for a in range(1, SHARES):

        @pl.when(z + a < SHARES)
        def _():
            group_copy(a).start()

    gate_in, filter_value = total(3), total(4)
    product = gate_in * filter_value
    pad[8 : 8 + length] = product

    halo = send(pad.at[pl.ds(length, 8)], pad.at[pl.ds(0, 8)], h_s, h_r, (after, tp))
    halo.start()
    gate_out = total(5)
    halo.wait_recv()
    edge = jnp.where(sp > 0, pad[0:8], 0.0)
    halo.wait_send()
    pad[0:8] = edge
    filtered = taps[TAPS - 1 : TAPS] * product
    for j in range(TAPS - 1):
        start = 8 - (TAPS - 1) + j
        filtered = filtered + taps[j : j + 1] * pad[start : start + length]
    filter_out = (gate_out * filtered).astype(BF16)

    for h in range(heads):
        sin[:, cuts[h]] = init[h].T
    for a in range(1, SHARES):

        @pl.when(z >= a)
        def _():
            group_landing(a).wait_recv()

    for i in range(SHARES - 1):

        @pl.when(i < z)
        def _():
            state, fall = parts_of(gland, i)
            sin[...] = jnp.exp(fall) * sin[...] + state

    incoming = (jnp.exp(near_decay) * sin[...] + near).astype(BF16)
    rec = []
    for h in range(heads):
        raw = within[h] + dot_on(query_in[:, cuts[h]], incoming[:, cuts[h]], 1, 1)
        scale = lax.rsqrt(jnp.mean(raw * raw, axis=-1, keepdims=True) + EPS)
        rec.append((raw * scale * hgain[...]).astype(BF16))
    rec_out = jnp.concatenate(rec, axis=-1)

    pltpu.make_async_copy(wof, vof, v_l.at[0]).wait()
    pltpu.make_async_copy(wor, vor, v_l.at[1]).wait()
    d_out = wof.shape[1]
    cols = d_out // CHUNKS

    def out_copy(c, b):
        to = (sp, shift_t(b))
        return send(obuf.at[c, shift_t(b)], oland.at[c, b], o_s.at[c, b], o_r.at[c, b], to)

    for c in range(CHUNKS):
        cut = slice(c * cols, (c + 1) * cols)
        part = dot(filter_out, vof[:, cut]) + dot(rec_out, vor[:, cut])
        obuf[c] = part.astype(BF16).reshape(n_tp, t_loc, cols)
        for b in range(1, n_tp):
            out_copy(c, b).start()
    for c in range(CHUNKS):
        s = obuf[c, tp].astype(F32)
        for b in range(1, n_tp):
            out_copy(c, b).wait_recv()
            s = s + oland[c, b].astype(F32)
        out[:, c * cols : (c + 1) * cols] = s.astype(BF16)

    for a, b in spread:
        token_copy(a, b).wait_send()
    for p in range(PROJ):
        repeat(group - 1, lambda i: weight_copy(p, i).wait_send())
        for a in range(1, SHARES):
            part_copy(p, a).wait_send()
    repeat(group - 1, lambda i: state_copy(i).wait_send())
    for a in range(1, SHARES):

        @pl.when(z + a < SHARES)
        def _():
            group_copy(a).wait_send()

    for c in range(CHUNKS):
        for b in range(1, n_tp):
            out_copy(c, b).wait_send()


def body(
    tokens,
    norm_gain,
    w_filter_b,
    w_filter_c,
    w_filter_v,
    filter_taps,
    w_query,
    retention_gate_matrix,
    w_input,
    forget_gap,
    additive_fade_log,
    head_gain,
    initial_state,
    w_out_filter,
    w_out_rec,
):
    n_sp, n_tp = lax.axis_size("sp"), lax.axis_size("tp")
    group = n_sp // SHARES
    t_loc, d = tokens.shape
    rows, width = w_query.shape
    depth = rows * group
    length = t_loc * n_tp
    d_out = w_out_filter.shape[1]
    cols = d_out // CHUNKS
    vmem = pl.BlockSpec(memory_space=pltpu.VMEM)
    hbm = pl.BlockSpec(memory_space=pl.ANY)
    peers = max(group - 1, 1)
    dma = pltpu.SemaphoreType.DMA
    return pl.pallas_call(
        functools.partial(mix_kernel, n_sp, n_tp),
        out_shape=jax.ShapeDtypeStruct((t_loc, d_out), BF16),
        in_specs=[vmem] * 7 + [hbm] * 8,
        out_specs=vmem,
        scratch_shapes=[
            pltpu.VMEM((SHARES, t_loc, depth), BF16),
            pltpu.VMEM((SHARES, n_tp, t_loc, depth), BF16),
            pltpu.VMEM((PROJ, depth, width), BF16),
            pltpu.VMEM((PROJ, SHARES, length, width), F32),
            pltpu.VMEM((PROJ, SHARES, length, width), BF16),
            pltpu.VMEM((PROJ, SHARES, length, width), BF16),
            pltpu.VMEM((group, HEAD_DIM + 16, width), BF16),
            pltpu.VMEM((SHARES, HEAD_DIM + 16, width), BF16),
            pltpu.VMEM((HEAD_DIM, width), F32),
            pltpu.VMEM((length + 8, width), F32),
            pltpu.VMEM((CHUNKS, n_tp, t_loc, cols), BF16),
            pltpu.VMEM((CHUNKS, n_tp, t_loc, cols), BF16),
            pltpu.VMEM(w_out_filter.shape, BF16),
            pltpu.VMEM(w_out_rec.shape, BF16),
            dma((SHARES, n_tp)),
            dma((SHARES, n_tp)),
            dma((PROJ,)),
            dma((PROJ, peers)),
            dma((PROJ, peers)),
            dma((PROJ, SHARES)),
            dma((PROJ, SHARES)),
            dma((peers,)),
            dma((peers,)),
            dma((SHARES,)),
            dma((SHARES,)),
            dma,
            dma,
            dma((CHUNKS, n_tp)),
            dma((CHUNKS, n_tp)),
            dma((2,)),
        ],
        compiler_params=pltpu.CompilerParams(
            collective_id=0, has_side_effects=True, vmem_limit_bytes=60 * 1024 * 1024
        ),
    )(
        tokens,
        norm_gain.reshape(1, d),
        filter_taps,
        forget_gap.reshape(1, width),
        additive_fade_log,
        head_gain.reshape(1, HEAD_DIM),
        initial_state,
        w_query,
        retention_gate_matrix,
        w_input,
        w_filter_c,
        w_filter_v,
        w_filter_b,
        w_out_filter,
        w_out_rec,
    )


def solution(mesh):
    placed = (
        P(("sp", "tp"), None),
        P(),
        P("sp", "tp"),
        P("sp", "tp"),
        P("sp", "tp"),
        P(None, "tp"),
        P("sp", "tp"),
        P("sp", "tp"),
        P("sp", "tp"),
        P("tp"),
        P("sp", "tp"),
        P(),
        P("tp", None, None),
        P("tp", None),
        P("tp", None),
    )
    return jax.shard_map(
        body, mesh=mesh, in_specs=placed, out_specs=P(("sp", "tp"), None), check_vma=False
    )
```

```python
import functools

import jax
import jax.numpy as jnp
from jax import lax
from jax.experimental import pallas as pl
from jax.experimental.pallas import tpu as pltpu
from jax.sharding import PartitionSpec as P

HEAD_DIM = 128
TAPS = 3
SHARES = 4
CHUNKS = 4
PROJ = 6
EPS = 1e-06
MESH = pl.DeviceIdType.MESH
F32 = jnp.float32
BF16 = jnp.bfloat16


def repeat(count, step):
    if count <= 4:
        for i in range(count):
            step(i)
    else:
        lax.fori_loop(0, count, lambda i, c: (step(i), c)[1], 0)


def dot(a, b):
    return jnp.dot(a, b, preferred_element_type=F32)


def dot_on(a, b, da, db):
    return lax.dot_general(a, b, (((da,), (db,)), ((), ())), preferred_element_type=F32)


def mix_kernel(
    n_sp,
    n_tp,
    tok,
    gain,
    taps,
    gap,
    fade,
    hgain,
    init,
    wq,
    wf,
    wi,
    wc,
    wv,
    wb,
    wof,
    wor,
    out,
    xs,
    xbuf,
    wbuf,
    own,
    psend,
    pland,
    sland,
    gland,
    sin,
    pad,
    obuf,
    oland,
    osend,
    acc,
    vof,
    vor,
    tok_s,
    tok_r,
    w_l,
    w_s,
    w_r,
    p_s,
    p_r,
    s_s,
    s_r,
    g_s,
    g_r,
    h_s,
    h_r,
    o_s,
    o_r,
    v_l,
):
    sp, tp = lax.axis_index("sp"), lax.axis_index("tp")
    group = n_sp // SHARES
    z, r = lax.div(sp, group), lax.rem(sp, group)
    t_loc = tok.shape[0]
    length = t_loc * n_tp
    rows, width = wq.shape
    depth = rows * group
    heads = width // HEAD_DIM
    weights = (wq, wf, wi, wc, wv, wb)

    def shift_z(by):
        return lax.rem(z + by + SHARES, SHARES)

    t_half, t_side = lax.div(tp, 2), lax.rem(tp, 2)
    mate = 2 * t_half + 1 - t_side
    across = 2 * (1 - t_half) + t_side
    corner = 2 * (1 - t_half) + 1 - t_side
    on_tp = (tp, mate, across, corner)

    def shift_r(by):
        return lax.rem(r + by + group, group)

    def send(src, dst, ss, rs, to):
        return pltpu.make_async_remote_copy(
            src_ref=src, dst_ref=dst, send_sem=ss, recv_sem=rs, device_id=to, device_id_type=MESH
        )

    barrier = pltpu.get_barrier_semaphore()

    def hail(a, b):
        pl.semaphore_signal(barrier, inc=1, device_id=(a, b), device_id_type=MESH)

    repeat(group - 1, lambda i: hail(z * group + shift_r(i + 1), tp))
    spread = [(a, b) for a in range(SHARES) for b in range(n_tp) if (a, b) != (0, 0)]
    for a, b in spread:
        hail(shift_z(a) * group + r, on_tp[b])
    after, before = lax.rem(sp + 1, n_sp), lax.rem(sp + n_sp - 1, n_sp)
    hail(after, tp)
    hail(before, tp)

    mine = pl.ds(pl.multiple_of(r * rows, rows), rows)
    for p in range(PROJ):
        pltpu.make_async_copy(weights[p], wbuf.at[p, mine], w_l.at[p]).start()
    pltpu.make_async_copy(wof, vof, v_l.at[0]).start()
    pltpu.make_async_copy(wor, vor, v_l.at[1]).start()

    x = tok[...].astype(F32)
    normed = x * lax.rsqrt(jnp.mean(x * x, axis=-1, keepdims=True) + EPS) * gain[...]
    normed = normed.astype(BF16)
    for a in range(SHARES):
        xs[a] = normed[:, a * depth : (a + 1) * depth]
    xbuf[z, tp] = xs[z]

    pl.semaphore_wait(barrier, group - 1 + len(spread) + 2)

    def token_copy(a, b):
        if b == 0:
            to = (shift_z(a) * group + r, tp)
            return send(xs.at[shift_z(a)], xbuf.at[z, tp], tok_s.at[a, b], tok_r.at[a, b], to)
        piece = xbuf.at[shift_z(-a), across if b == 3 else tp]
        to = across if b == 2 else mate
        return send(piece, piece, tok_s.at[a, b], tok_r.at[a, b], (sp, to))

    def token_landing(a, b):
        piece = xbuf.at[shift_z(-a), on_tp[b]]
        if b == 0:
            to = (shift_z(-a) * group + r, tp)
            return send(xs.at[0], piece, tok_s.at[a, b], tok_r.at[a, b], to)
        frm = across if b == 2 else mate
        return send(piece, piece, tok_s.at[a, b], tok_r.at[a, b], (sp, frm))

    def weight_copy(p, i):
        to = (z * group + shift_r(i + 1), tp)
        return send(weights[p], wbuf.at[p, mine], w_s.at[p, i], w_r.at[p, i], to)

    def weight_landing(p, i):
        src = shift_r(-i - 1)
        theirs = pl.ds(pl.multiple_of(src * rows, rows), rows)
        return send(
            weights[p], wbuf.at[p, theirs], w_s.at[p, i], w_r.at[p, i], (z * group + src, tp)
        )

    for a in (2, 1, 3):
        token_copy(a, 0).start()
    for b in (2, 1):
        token_copy(0, b).start()
    for p in range(PROJ):
        repeat(group - 1, lambda i: weight_copy(p, i).start())
    for a in (1, 3, 2):
        token_landing(a, 0).wait_recv()
        for b in (2, 1):
            token_copy(a, b).start()
    for a in (0, 1, 3, 2):
        token_landing(a, 2).wait_recv()
        token_copy(a, 3).start()
    for a in (0, 1, 3, 2):
        for b in (1, 3):
            token_landing(a, b).wait_recv()

    half, side = lax.div(z, 2), lax.rem(z, 2)
    near_z = 2 * half + 1 - side
    far_z = 2 * (1 - half) + side

    def part_copy(p, k):
        to = ((near_z if k < 2 else far_z) * group + r, tp)
        return send(psend.at[p, k], pland.at[p, k], p_s.at[p, k], p_r.at[p, k], to)

    def project(p):
        pltpu.make_async_copy(weights[p], wbuf.at[p, mine], w_l.at[p]).wait()
        repeat(group - 1, lambda i: weight_landing(p, i).wait_recv())
        full = xbuf[...].reshape(SHARES * length, depth)
        own[p] = dot(full, wbuf[p]).reshape(SHARES, length, width)
        psend[p, 0] = own[p, 2 * (1 - half) + 1 - side].astype(BF16)
        part_copy(p, 0).start()
        psend[p, 1] = own[p, near_z].astype(BF16)
        part_copy(p, 1).start()

    def relay(p):
        part_copy(p, 0).wait_recv()
        psend[p, 2] = (own[p, far_z] + pland[p, 0].astype(F32)).astype(BF16)
        part_copy(p, 2).start()

    def total(p):
        part_copy(p, 1).wait_recv()
        part_copy(p, 2).wait_recv()
        s = own[p, z] + pland[p, 1].astype(F32) + pland[p, 2].astype(F32)
        return s.astype(BF16).astype(F32)

    for p in range(PROJ):
        project(p)
        if 0 < p < PROJ - 1:
            relay(p - 1)

    query, logit, value = total(0), total(1), total(2)
    rate = gap[...] / (1.0 + jnp.exp(logit))
    decay = jnp.log1p(-rate) + fade[...]
    value = (value / (1.0 + jnp.exp(-value))).astype(BF16)
    below = lax.broadcasted_iota(jnp.int32, (length, length), 0) >= lax.broadcasted_iota(
        jnp.int32, (length, length), 1
    )
    running = jnp.dot(
        below.astype(F32), decay, preferred_element_type=F32, precision=lax.Precision.HIGHEST
    )
    middle = running[length // 2 - 1 : length // 2]
    last = running[length - 1 : length]
    query_mid = (query * jnp.exp(running - middle)).astype(BF16)
    key_mid = (rate * jnp.exp(middle - running)).astype(BF16)
    key_end = (rate * jnp.exp(last - running)).astype(BF16)
    query_in = (query * jnp.exp(running)).astype(BF16)
    within = []
    cuts = [slice(h * HEAD_DIM, (h + 1) * HEAD_DIM) for h in range(heads)]
    for cut in cuts:
        sland[r, 0:HEAD_DIM, cut] = dot_on(value[:, cut], key_end[:, cut], 0, 0).astype(BF16)
    coarse = last.astype(BF16).astype(F32)
    upper = lax.broadcasted_iota(jnp.int32, (16, width), 0) < 8
    sland[r, HEAD_DIM : HEAD_DIM + 16, :] = jnp.where(upper, coarse, last - coarse).astype(BF16)

    def state_copy(i):
        to = (z * group + shift_r(i + 1), tp)
        return send(sland.at[r], sland.at[r], s_s.at[i], s_r.at[i], to)

    def state_landing(i):
        src = shift_r(-i - 1)
        return send(sland.at[src], sland.at[src], s_s.at[i], s_r.at[i], (z * group + src, tp))

    repeat(group - 1, lambda i: state_copy(i).start())
    relay(4)
    for cut in cuts:
        scores = dot_on(query_mid[:, cut], key_mid[:, cut], 1, 1)
        scores = jnp.where(below, scores, 0.0).astype(BF16)
        within.append(dot(scores, value[:, cut]))

    relay(5)

    repeat(group - 1, lambda i: state_landing(i).wait_recv())

    def parts_of(ref, i):
        tail = ref[i, HEAD_DIM : HEAD_DIM + 16, :].astype(F32)
        return ref[i, 0:HEAD_DIM, :].astype(F32), tail[0:1] + tail[8:9]

    def join(i, carry):
        whole, whole_decay, near, near_decay = carry
        state, fall = parts_of(sland, i)
        factor = jnp.exp(fall)
        whole, whole_decay = factor * whole + state, whole_decay + fall
        earlier = i < r
        near = jnp.where(earlier, factor * near + state, near)
        near_decay = jnp.where(earlier, near_decay + fall, near_decay)
        return whole, whole_decay, near, near_decay

    blank = jnp.zeros((HEAD_DIM, width), F32)
    line = jnp.zeros((1, width), F32)
    carry = (blank, line, blank, line)
    if group <= 4:
        for i in range(group):
            carry = join(i, carry)
    else:
        carry = lax.fori_loop(0, group, join, carry)
    whole, whole_decay, near, near_decay = carry
    gland[z, 0:HEAD_DIM, :] = whole.astype(BF16)
    coarse = whole_decay.astype(BF16).astype(F32)
    gland[z, HEAD_DIM : HEAD_DIM + 16, :] = jnp.where(upper, coarse, whole_decay - coarse).astype(
        BF16
    )

    def group_copy(a):
        return send(
            gland.at[z], gland.at[z], g_s.at[a], g_r.at[a], (shift_z(a) * group + r, tp)
        )

    def group_landing(a):
        src = shift_z(-a)
        return send(gland.at[src], gland.at[src], g_s.at[a], g_r.at[a], (src * group + r, tp))

    for a in range(1, SHARES):

        @pl.when(z + a < SHARES)
        def _():
            group_copy(a).start()

    gate_in, filter_value = total(3), total(4)
    product = gate_in * filter_value
    pad[8 : 8 + length] = product

    halo = send(pad.at[pl.ds(length, 8)], pad.at[pl.ds(0, 8)], h_s, h_r, (after, tp))
    halo.start()

    for h in range(heads):
        sin[:, cuts[h]] = init[h].T
    for a in range(1, SHARES):

        @pl.when(z >= a)
        def _():
            group_landing(a).wait_recv()

    for i in range(SHARES - 1):

        @pl.when(i < z)
        def _():
            state, fall = parts_of(gland, i)
            sin[...] = jnp.exp(fall) * sin[...] + state

    incoming = (jnp.exp(near_decay) * sin[...] + near).astype(BF16)
    rec = []
    for h in range(heads):
        raw = within[h] + dot_on(query_in[:, cuts[h]], incoming[:, cuts[h]], 1, 1)
        scale = lax.rsqrt(jnp.mean(raw * raw, axis=-1, keepdims=True) + EPS)
        rec.append((raw * scale * hgain[...]).astype(BF16))
    rec_out = jnp.concatenate(rec, axis=-1)

    d_out = wof.shape[1]
    pltpu.make_async_copy(wor, vor, v_l.at[1]).wait()
    acc[...] = dot(rec_out, vor[...])

    gate_out = total(5)
    halo.wait_recv()
    edge = jnp.where(sp > 0, pad[0:8], 0.0)
    halo.wait_send()
    pad[0:8] = edge
    filtered = taps[TAPS - 1 : TAPS] * product
    for j in range(TAPS - 1):
        start = 8 - (TAPS - 1) + j
        filtered = filtered + taps[j : j + 1] * pad[start : start + length]
    filter_out = (gate_out * filtered).astype(BF16)

    pltpu.make_async_copy(wof, vof, v_l.at[0]).wait()
    cols = d_out // CHUNKS

    def out_copy(c, k):
        src = (obuf.at[c, corner], obuf.at[c, mate], osend.at[c])[k]
        to = (sp, across if k == 2 else mate)
        return send(src, oland.at[c, k], o_s.at[c, k], o_r.at[c, k], to)

    def out_relay(c):
        out_copy(c, 0).wait_recv()
        osend[c] = (obuf[c, across].astype(F32) + oland[c, 0].astype(F32)).astype(BF16)
        out_copy(c, 2).start()

    for c in range(CHUNKS):
        cut = slice(c * cols, (c + 1) * cols)
        part = dot(filter_out, vof[:, cut]) + acc[:, cut]
        obuf[c] = part.astype(BF16).reshape(n_tp, t_loc, cols)
        out_copy(c, 0).start()
        out_copy(c, 1).start()
        if c > 0:
            out_relay(c - 1)
    out_relay(CHUNKS - 1)
    for c in range(CHUNKS):
        s = obuf[c, tp].astype(F32)
        for k in (1, 2):
            out_copy(c, k).wait_recv()
            s = s + oland[c, k].astype(F32)
        out[:, c * cols : (c + 1) * cols] = s.astype(BF16)

    for a, b in spread:
        token_copy(a, b).wait_send()
    for p in range(PROJ):
        repeat(group - 1, lambda i: weight_copy(p, i).wait_send())
        for k in range(3):
            part_copy(p, k).wait_send()
    repeat(group - 1, lambda i: state_copy(i).wait_send())
    for a in range(1, SHARES):

        @pl.when(z + a < SHARES)
        def _():
            group_copy(a).wait_send()

    for c in range(CHUNKS):
        for k in range(3):
            out_copy(c, k).wait_send()


def body(
    tokens,
    norm_gain,
    w_filter_b,
    w_filter_c,
    w_filter_v,
    filter_taps,
    w_query,
    retention_gate_matrix,
    w_input,
    forget_gap,
    additive_fade_log,
    head_gain,
    initial_state,
    w_out_filter,
    w_out_rec,
):
    n_sp, n_tp = lax.axis_size("sp"), lax.axis_size("tp")
    group = n_sp // SHARES
    t_loc, d = tokens.shape
    rows, width = w_query.shape
    depth = rows * group
    length = t_loc * n_tp
    d_out = w_out_filter.shape[1]
    cols = d_out // CHUNKS
    vmem = pl.BlockSpec(memory_space=pltpu.VMEM)
    hbm = pl.BlockSpec(memory_space=pl.ANY)
    peers = max(group - 1, 1)
    dma = pltpu.SemaphoreType.DMA
    return pl.pallas_call(
        functools.partial(mix_kernel, n_sp, n_tp),
        out_shape=jax.ShapeDtypeStruct((t_loc, d_out), BF16),
        in_specs=[vmem] * 7 + [hbm] * 8,
        out_specs=vmem,
        scratch_shapes=[
            pltpu.VMEM((SHARES, t_loc, depth), BF16),
            pltpu.VMEM((SHARES, n_tp, t_loc, depth), BF16),
            pltpu.VMEM((PROJ, depth, width), BF16),
            pltpu.VMEM((PROJ, SHARES, length, width), F32),
            pltpu.VMEM((PROJ, 3, length, width), BF16),
            pltpu.VMEM((PROJ, 3, length, width), BF16),
            pltpu.VMEM((group, HEAD_DIM + 16, width), BF16),
            pltpu.VMEM((SHARES, HEAD_DIM + 16, width), BF16),
            pltpu.VMEM((HEAD_DIM, width), F32),
            pltpu.VMEM((length + 8, width), F32),
            pltpu.VMEM((CHUNKS, n_tp, t_loc, cols), BF16),
            pltpu.VMEM((CHUNKS, 3, t_loc, cols), BF16),
            pltpu.VMEM((CHUNKS, t_loc, cols), BF16),
            pltpu.VMEM((length, d_out), F32),
            pltpu.VMEM(w_out_filter.shape, BF16),
            pltpu.VMEM(w_out_rec.shape, BF16),
            dma((SHARES, n_tp)),
            dma((SHARES, n_tp)),
            dma((PROJ,)),
            dma((PROJ, peers)),
            dma((PROJ, peers)),
            dma((PROJ, 3)),
            dma((PROJ, 3)),
            dma((peers,)),
            dma((peers,)),
            dma((SHARES,)),
            dma((SHARES,)),
            dma,
            dma,
            dma((CHUNKS, 3)),
            dma((CHUNKS, 3)),
            dma((2,)),
        ],
        compiler_params=pltpu.CompilerParams(
            collective_id=0, has_side_effects=True, vmem_limit_bytes=60 * 1024 * 1024
        ),
    )(
        tokens,
        norm_gain.reshape(1, d),
        filter_taps,
        forget_gap.reshape(1, width),
        additive_fade_log,
        head_gain.reshape(1, HEAD_DIM),
        initial_state,
        w_query,
        retention_gate_matrix,
        w_input,
        w_filter_c,
        w_filter_v,
        w_filter_b,
        w_out_filter,
        w_out_rec,
    )


def solution(mesh):
    placed = (
        P(("sp", "tp"), None),
        P(),
        P("sp", "tp"),
        P("sp", "tp"),
        P("sp", "tp"),
        P(None, "tp"),
        P("sp", "tp"),
        P("sp", "tp"),
        P("sp", "tp"),
        P("tp"),
        P("sp", "tp"),
        P(),
        P("tp", None, None),
        P("tp", None),
        P("tp", None),
    )
    return jax.shard_map(
        body, mesh=mesh, in_specs=placed, out_specs=P(("sp", "tp"), None), check_vma=False
    )
```
